32 devices in a mesh: fs: 8 (over z, x), tp: 4 (over y, core).
Axes of the slice: x: 2, y: 2, z: 4, core: 2. Of those that a mesh axis runs over, the one named last changes fastest.
Arguments:
- normed_input: bfloat16 [16384, 2048], P('fs'), may hold values from -6 to 6
- gate_cotangent: bfloat16 [16384, 2048], P('fs', 'tp'), may hold values from -0.125 to 0.125
- first_value_cot: bfloat16 [16384, 1024], P('fs', 'tp'), may hold values from -0.125 to 0.125
- second_value_cot: bfloat16 [16384, 1024], P('fs', 'tp'), may hold values from -0.125 to 0.125
- head_lambda: float32 [8], P('tp'), may hold values from 0.3 to 0.8
- projection: bfloat16 [2048, 256], replicated, may hold values from -1 to 1, as said below
- gate_weight: float32 [2048, 2048], P('fs', 'tp'), may hold values from -0.125 to 0.125
- gate_first: float32 [256, 2048], P('fs', 'tp'), may hold values from -1.5 to 1.5
- gate_second: float32 [256, 2048], P('fs', 'tp'), may hold values from 0.01 to 1
- value_weight: float32 [2048, 1024], P('fs', 'tp'), may hold values from -0.125 to 0.125
- value_first: float32 [256, 1024], P('fs', 'tp'), may hold values from -1.5 to 1.5
- value_second: float32 [256, 1024], P('fs', 'tp'), may hold values from 0.01 to 1
Outputs:
- new_gate_weight: float32 [2048, 2048], P('fs', 'tp')
- gate_step: float32 [2048, 2048], P('fs', 'tp')
- gate_copy: bfloat16 [2048, 2048], P(None, 'tp')
- new_gate_first: float32 [256, 2048], P('fs', 'tp')
- new_gate_second: float32 [256, 2048], P('fs', 'tp')
- new_value_weight: float32 [2048, 1024], P('fs', 'tp')
- value_step: float32 [2048, 1024], P('fs', 'tp')
- value_copy: bfloat16 [2048, 1024], P(None, 'tp')
- new_value_first: float32 [256, 1024], P('fs', 'tp')
- new_value_second: float32 [256, 1024], P('fs', 'tp')
The draws below stay inside these ranges and needn't reach their ends.
Inputs may be any that keep to these rules, and one draw needn't show every extreme that they name: `projection`: a low-rank factor whose rows differ in scale.
All inputs are finite; a program needn't handle non-finite values.
Results may differ from the reference program's by a relative error of at most 0.0054.
Values may be sent and summed in bfloat16 or wider, within the bound.
A program may use at most 64 MiB of HBM per device.

```python
import math
import jax
import jax.numpy as jnp
from jax import lax

D = 2048
HEADS = 8
VDIM = 128
RANK = 256
TOKENS = 16384


def draw_projection(key, part):
    noise_key = jax.random.fold_in(key, 11)
    rough_key = jax.random.fold_in(key, 12)
    phase_key = jax.random.fold_in(key, 13)
    row_place = jnp.arange(D, dtype=jnp.float32)[:, None] / D
    phase = jax.random.uniform(phase_key, (), jnp.float32, 0.0, 6.2832)
    slow = jnp.exp(1.2 * jnp.sin(12.566 * row_place + phase))
    rough = jnp.exp(jax.random.uniform(rough_key, (D, 1), jnp.float32, -0.5, 0.5))
    base = jax.random.normal(noise_key, (D, RANK), jnp.float32)
    value = base * slow * rough * D ** (-0.5)
    return jnp.clip(value, -1.0, 1.0).astype(jnp.bfloat16)


def raised(entries, key, source, target, shards_of, factor):
    owner, partner = [(jnp.arange(entries.shape[axis_at]) // (entries.shape[axis_at] // shards_of)).reshape([-1 if axis == axis_at else 1 for axis in range(entries.ndim)]) for axis_at in (source, target)]
    chosen = jax.random.permutation(key, shards_of)[partner]
    strong = (owner == chosen) | (owner == (partner + shards_of // 2) % shards_of)
    return jnp.where(strong, factor * entries, entries)


def steps_of(key, dims, split, smallest, largest):
    loudness = 1.0
    for axis_at, blocks in split:
        heights = jax.random.uniform(jax.random.fold_in(jax.random.fold_in(key, 6), axis_at), (blocks,), jnp.float32, smallest / len(split), largest / len(split))
        loudness = loudness * jnp.repeat(jnp.exp(heights), dims[axis_at] // blocks).reshape((-1,) + (1,) * (len(dims) - 1 - axis_at))
    return loudness


def noise(own_key, dims, spread, bound, cuts=(), held_as=jnp.bfloat16):
    array = spread * jax.random.normal(own_key, dims, jnp.float32)
    if cuts:
        array = array * steps_of(own_key, dims, cuts, -0.22, 0.18)
    return jnp.clip(array, -bound, bound).astype(held_as)


def gaussian_with(key, extent, deviation, limit, shards, heavy, kind=jnp.bfloat16):
    array = deviation * jax.random.normal(key, extent, jnp.float32)
    if shards:
        array = array * steps_of(key, extent, shards, -0.22, 0.18)
    return jnp.clip(raised(array, jax.random.fold_in(key, 3), *heavy), -limit, limit).astype(kind)


def setup_inputs(seed: int = 0) -> dict:
    splits = jax.random.split(jax.random.key(seed), 13)
    return {
        "normed_input": gaussian_with(splits[0], (TOKENS, D), 1.0, 6.0, ((0, 8),), (0, 1, 8, 2.0)),
        "gate_cotangent": noise(splits[1], (TOKENS, D), (TOKENS ** -0.5), 0.125, ((0, 8), (1, 4))),
        "first_value_cot": noise(splits[2], (TOKENS, HEADS * VDIM), (TOKENS ** -0.5), 0.125, ((0, 8), (1, 4))),
        "second_value_cot": noise(splits[3], (TOKENS, HEADS * VDIM), (TOKENS ** -0.5), 0.125, ((0, 8), (1, 4))),
        "head_lambda": jnp.clip(0.3 + 0.5 * jax.random.uniform(splits[4], (HEADS,), jnp.float32) ** steps_of(splits[4], (HEADS,), ((0, 4),), -0.2, 0.2), 0.3, 0.8),
        "projection": draw_projection(jax.random.fold_in(splits[12], 71), 0),
        "gate_weight": noise(splits[6], (D, D), D ** -0.5, 0.125, ((0, 8), (1, 4)), jnp.float32),
        "gate_first": noise(splits[7], (RANK, D), 0.1, 1.5, ((0, 8), (1, 4)), jnp.float32),
        "gate_second": jnp.clip(jnp.exp(math.log(1.0) - 4.6051702 * jax.random.uniform(splits[8], (RANK, D), jnp.float32) ** steps_of(splits[8], (RANK, D), ((0, 8), (1, 4)), -0.2, 0.2)), 0.01, 1.0),
        "value_weight": noise(splits[9], (D, HEADS * VDIM), D ** -0.5, 0.125, ((0, 8), (1, 4)), jnp.float32),
        "value_first": noise(splits[10], (RANK, HEADS * VDIM), 0.1, 1.5, ((0, 8), (1, 4)), jnp.float32),
        "value_second": jnp.clip(jnp.exp(math.log(1.0) - 4.6051702 * jax.random.uniform(splits[11], (RANK, HEADS * VDIM), jnp.float32) ** steps_of(splits[11], (RANK, HEADS * VDIM), ((0, 8), (1, 4)), -0.2, 0.2)), 0.01, 1.0),
    }


moment_decay = 0.9
square_decay = 0.95
adam_floor = 1e-08
learn_rate = 0.02
rms_floor = 0.1

def across_tokens(left, right):
    return lax.dot_general(left, right, (((0,), (0,)), ((), ())), preferred_element_type=jnp.float32)

def optimizer_step(weight, first, second, gradient, projection):
    factor = projection.astype(jnp.float32)
    low = lax.dot_general(factor, gradient, (((0,), (0,)), ((), ())), precision=lax.Precision.HIGHEST)
    new_first = moment_decay * first + (1.0 - moment_decay) * low
    new_second = square_decay * second + (1.0 - square_decay) * low * low
    direction = new_first / (jnp.sqrt(new_second) + adam_floor)
    update = jnp.dot(factor, direction, precision=lax.Precision.HIGHEST)
    step = update / (jnp.sqrt(jnp.mean(update * update)) + rms_floor)
    new_weight = weight - learn_rate * step
    return (new_weight, step, new_weight.astype(jnp.bfloat16), new_first, new_second)

def reference(normed_input, gate_cotangent, first_value_cot, second_value_cot, head_lambda, projection, gate_weight, gate_first, gate_second, value_weight, value_first, value_second):
    column_lambda = jnp.repeat(head_lambda, VDIM)
    value_cot = (first_value_cot.astype(jnp.float32) - column_lambda[None, :] * second_value_cot.astype(jnp.float32)).astype(jnp.bfloat16)
    gate_grad = across_tokens(normed_input, gate_cotangent)
    value_grad = across_tokens(normed_input, value_cot)
    gate_parts = optimizer_step(gate_weight, gate_first, gate_second, gate_grad, projection)
    value_parts = optimizer_step(value_weight, value_first, value_second, value_grad, projection)
    return (gate_parts[0], gate_parts[1], gate_parts[2], gate_parts[3], gate_parts[4], value_parts[0], value_parts[1], value_parts[2], value_parts[3], value_parts[4])
```

```python
import functools

import jax
import jax.numpy as jnp
from jax import lax
from jax.experimental import pallas as pl
from jax.experimental.pallas import tpu as pltpu
from jax.sharding import PartitionSpec as P

VDIM = 128
PIECES = 4
CHUNKS = 4
STEP_TOKENS = 256

moment_decay = 0.9
square_decay = 0.95
adam_floor = 1e-08
learn_rate = 0.02
rms_floor = 0.1

MESH = pl.DeviceIdType.MESH
f32, bf16 = jnp.float32, jnp.bfloat16


def factor_fs(count):
    inner = 1
    while (2 * inner) ** 2 <= count and count % (2 * inner) == 0:
        inner *= 2
    return count // inner, inner


def kernel(
    nz,
    nx,
    nt,
    x_hbm,
    gcot_hbm,
    fcot_hbm,
    scot_hbm,
    lam_ref,
    proj_hbm,
    gw_hbm,
    gm_hbm,
    gs_hbm,
    vw_hbm,
    vm_hbm,
    vs_hbm,
    ngw_hbm,
    gstep_hbm,
    gcopy_hbm,
    ngm_hbm,
    ngs_hbm,
    nvw_hbm,
    vstep_hbm,
    vcopy_hbm,
    nvm_hbm,
    nvs_hbm,
    xv,
    gcv,
    fcv,
    scv,
    pv,
    gw,
    vw,
    gm,
    gs,
    vm,
    vs,
    wall,
    acc,
    rsrc,
    rsx,
    zsrc,
    rsz,
    dall,
    dcat,
    upd,
    sums,
    gcs,
    vcs,
    gsteps,
    vsteps,
    in_sem,
    x_sem,
    out_sem,
    copy_sem,
    wz_send,
    wz_recv,
    wx_send,
    wx_recv,
    rx_send,
    rx_recv,
    rz_send,
    rz_recv,
    dz_send,
    dz_recv,
    dx_send,
    dx_recv,
    t_send,
    t_recv,
):
    nfs = nz * nx
    f = lax.axis_index("fs")
    t = lax.axis_index("tp")
    z = lax.div(f, nx)
    x = lax.rem(f, nx)
    rows, cg = gw.shape
    cv = vw.shape[1]
    cols = cg + cv
    rank = acc.shape[0]
    share = rank // nfs
    part = rows // PIECES
    tokens = x_hbm.shape[0] // CHUNKS

    def zpeer(k):
        return lax.rem(z + k, nz)

    def xpeer(k):
        return lax.rem(x + k, nx)

    barrier = pltpu.get_barrier_semaphore()
    for k in range(1, nz):
        pl.semaphore_signal(barrier, inc=1, device_id=(zpeer(k) * nx + x, t), device_id_type=MESH)
    for k in range(1, nx):
        pl.semaphore_signal(barrier, inc=1, device_id=(z * nx + xpeer(k), t), device_id_type=MESH)
    for k in range(1, nt):
        pl.semaphore_signal(barrier, inc=1, device_id=(f, lax.rem(t + k, nt)), device_id_type=MESH)

    small = [
        pltpu.make_async_copy(src, dst, in_sem.at[i])
        for i, (src, dst) in enumerate(
            [
                (gw_hbm, gw),
                (vw_hbm, vw),
                (proj_hbm, pv),
                (gm_hbm, gm),
                (gs_hbm, gs),
                (vm_hbm, vm),
                (vs_hbm, vs),
            ]
        )
    ]

    def chunk_copies(c):
        at = pl.ds(c * tokens, tokens)
        return [
            pltpu.make_async_copy(src.at[at], dst.at[at], x_sem.at[i, c])
            for i, (src, dst) in enumerate(
                [(x_hbm, xv), (gcot_hbm, gcv), (fcot_hbm, fcv), (scot_hbm, scv)]
            )
        ]

    for i in range(3):
        small[i].start()
    for c in range(CHUNKS):
        for copy in chunk_copies(c):
            copy.start()
    for i in range(3, 7):
        small[i].start()

    small[0].wait()
    small[1].wait()
    for p in range(PIECES):
        at = pl.ds(p * part, part)
        wall[f, p, :, :cg] = gw[at, :].astype(bf16)
        wall[f, p, :, cg:] = vw[at, :].astype(bf16)

    def wz(k, p, src_z):
        owner = src_z * nx + x
        return pltpu.make_async_remote_copy(
            src_ref=wall.at[owner, p],
            dst_ref=wall.at[owner, p],
            send_sem=wz_send.at[k, p],
            recv_sem=wz_recv.at[src_z, p],
            device_id=(zpeer(k) * nx + x, t),
            device_id_type=MESH,
        )

    def wx(k, p, src_z, src_x):
        owner = src_z * nx + src_x
        return pltpu.make_async_remote_copy(
            src_ref=wall.at[owner, p],
            dst_ref=wall.at[owner, p],
            send_sem=wx_send.at[k, src_z, p],
            recv_sem=wx_recv.at[src_x, src_z, p],
            device_id=(z * nx + xpeer(k), t),
            device_id_type=MESH,
        )

    def send_z(p):
        for k in range(1, nz):
            wz(k, p, z).start()

    def relay(p):
        for k in range(1, nz):
            wz(k, p, zpeer(k)).wait_recv()
            for m in range(1, nx):
                wx(m, p, zpeer(k), x).start()

    pl.semaphore_wait(barrier, (nz - 1) + (nx - 1) + (nt - 1))
    send_z(0)
    for p in range(PIECES):
        for k in range(1, nx):
            wx(k, p, z, x).start()

    small[2].wait()
    acc[...] = jnp.zeros_like(acc)
    for c in range(CHUNKS):
        for copy in chunk_copies(c):
            copy.wait()

        def multiply(i, carry):
            at = pl.ds(pl.multiple_of(c * tokens + i * STEP_TOKENS, STEP_TOKENS), STEP_TOKENS)
            upper = jnp.dot(xv[at, :], pv[...], preferred_element_type=f32).astype(bf16)
            lam = lam_ref[...]
            value = (fcv[at, :].astype(f32) - lam * scv[at, :].astype(f32)).astype(bf16)
            over = (((0,), (0,)), ((), ()))
            acc[:, :cg] += lax.dot_general(upper, gcv[at, :], over, preferred_element_type=f32)
            acc[:, cg:] += lax.dot_general(upper, value, over, preferred_element_type=f32)
            return carry

        lax.fori_loop(0, tokens // STEP_TOKENS, multiply, 0)

    for zi in range(nz):
        for xi in range(nx):
            at = pl.ds((zi * nx + xi) * share, share)
            rsrc[xi, zi] = acc[at, :].astype(bf16)

    def rx(k, src_x, dst_x):
        return pltpu.make_async_remote_copy(
            src_ref=rsrc.at[dst_x],
            dst_ref=rsx.at[src_x],
            send_sem=rx_send.at[k],
            recv_sem=rx_recv.at[src_x],
            device_id=(z * nx + xpeer(k), t),
            device_id_type=MESH,
        )

    for k in range(1, nx):
        rx(k, x, xpeer(k)).start()
    send_z(1)
    relay(0)
    for k in range(1, nx):
        rx(k, xpeer(k), x).wait_recv()
    for zi in range(nz):
        at = pl.ds(pl.multiple_of((zi * nx + x) * share, share), share)
        total = acc[at, :]
        for k in range(1, nx):
            total = total + rsx[xpeer(k), zi].astype(f32)
        zsrc[zi] = total.astype(bf16)

    def rz(k, src_z, dst_z):
        return pltpu.make_async_remote_copy(
            src_ref=zsrc.at[dst_z],
            dst_ref=rsz.at[src_z],
            send_sem=rz_send.at[k],
            recv_sem=rz_recv.at[src_z],
            device_id=(zpeer(k) * nx + x, t),
            device_id_type=MESH,
        )

    for k in range(1, nz):
        rz(k, z, zpeer(k)).start()
    send_z(2)
    relay(1)
    for i in range(3, 7):
        small[i].wait()
    low = zsrc[z].astype(f32)
    for k in range(1, nz):
        rz(k, zpeer(k), z).wait_recv()
        low = low + rsz[zpeer(k)].astype(f32)

    for first, second, at in ((gm, gs, slice(0, cg)), (vm, vs, slice(cg, cols))):
        mine = low[:, at]
        new_first = moment_decay * first[...] + (1.0 - moment_decay) * mine
        new_second = square_decay * second[...] + (1.0 - square_decay) * mine * mine
        first[...] = new_first
        second[...] = new_second
        dall[f, :, at] = (new_first / (jnp.sqrt(new_second) + adam_floor)).astype(bf16)

    outs = [
        pltpu.make_async_copy(src, dst, out_sem.at[i])
        for i, (src, dst) in enumerate(
            [
                (gm, ngm_hbm),
                (gs, ngs_hbm),
                (vm, nvm_hbm),
                (vs, nvs_hbm),
                (gw, ngw_hbm),
                (vw, nvw_hbm),
                (gsteps, gstep_hbm),
                (vsteps, vstep_hbm),
            ]
        )
    ]
    for i in range(4):
        outs[i].start()

    def dz(k, src_z):
        owner = src_z * nx + x
        return pltpu.make_async_remote_copy(
            src_ref=dall.at[owner],
            dst_ref=dall.at[owner],
            send_sem=dz_send.at[k],
            recv_sem=dz_recv.at[src_z],
            device_id=(zpeer(k) * nx + x, t),
            device_id_type=MESH,
        )

    def dx(k, src_z, src_x):
        owner = src_z * nx + src_x
        return pltpu.make_async_remote_copy(
            src_ref=dall.at[owner],
            dst_ref=dall.at[owner],
            send_sem=dx_send.at[k, src_z],
            recv_sem=dx_recv.at[src_x, src_z],
            device_id=(z * nx + xpeer(k), t),
            device_id_type=MESH,
        )

    for k in range(1, nz):
        dz(k, z).start()
    for m in range(1, nx):
        dx(m, z, x).start()
    send_z(3)
    relay(2)
    for k in range(1, nz):
        dz(k, zpeer(k)).wait_recv()
        for m in range(1, nx):
            dx(m, zpeer(k), x).start()
    for m in range(1, nx):
        for zi in range(nz):
            dx(m, zi, xpeer(m)).wait_recv()

    for j in range(nfs):
        dcat[pl.ds(j * share, share), :] = dall[j].astype(f32)
    direction = dcat[...].astype(bf16)

    def expand(j, squares):
        left = pv[pl.ds(pl.multiple_of(j * rows, rows), rows), :]
        block = jnp.dot(left, direction, preferred_element_type=f32)
        upd[j] = block
        return squares + jnp.sum(block * block, axis=0, keepdims=True)

    squares = lax.fori_loop(0, nfs, expand, jnp.zeros((1, cols), f32))
    gate_sum = jnp.sum(squares[:, :cg], axis=1, keepdims=True)
    value_sum = jnp.sum(squares[:, cg:], axis=1, keepdims=True)
    sums[t, 0] = jnp.broadcast_to(gate_sum, (8, 128))
    sums[t, 1] = jnp.broadcast_to(value_sum, (8, 128))

    def tp(k, src_t):
        return pltpu.make_async_remote_copy(
            src_ref=sums.at[src_t],
            dst_ref=sums.at[src_t],
            send_sem=t_send.at[k],
            recv_sem=t_recv.at[src_t],
            device_id=(f, lax.rem(t + k, nt)),
            device_id_type=MESH,
        )

    for k in range(1, nt):
        tp(k, t).start()
    relay(3)
    for k in range(1, nt):
        tp(k, lax.rem(t + k, nt)).wait_recv()
    whole = sums[0]
    for k in range(1, nt):
        whole = whole + sums[k]
    entries = nfs * rows * nt
    gscale = (1.0 / (jnp.sqrt(whole[0] / (entries * cg)) + rms_floor))[0:1, 0:1]
    vscale = (1.0 / (jnp.sqrt(whole[1] / (entries * cv)) + rms_floor))[0:1, 0:1]

    gstep = upd[f, :, :cg] * gscale
    vstep = upd[f, :, cg:] * vscale
    gsteps[...] = gstep
    vsteps[...] = vstep
    gw[...] = gw[...] - learn_rate * gstep
    vw[...] = vw[...] - learn_rate * vstep
    for i in range(4, 8):
        outs[i].start()

    copies = []
    for p in range(PIECES):
        for m in range(1, nx):
            for zi in range(nz):
                wx(m, p, zi, xpeer(m)).wait_recv()
        at = pl.ds(p * part, part)

        def finish(j, carry):
            gcs[j, p] = (wall[j, p, :, :cg].astype(f32) - learn_rate * (upd[j, at, :cg] * gscale)).astype(bf16)
            vcs[j, p] = (wall[j, p, :, cg:].astype(f32) - learn_rate * (upd[j, at, cg:] * vscale)).astype(bf16)
            return carry

        lax.fori_loop(0, nfs, finish, 0)
        for i, (src, dst) in enumerate([(gcs, gcopy_hbm), (vcs, vcopy_hbm)]):
            copies.append(pltpu.make_async_copy(src.at[:, p], dst.at[:, p], copy_sem.at[i, p]))
            copies[-1].start()

    for copy in copies + outs:
        copy.wait()
    for k in range(1, nz):
        for p in range(PIECES):
            wz(k, p, z).wait_send()
        rz(k, z, zpeer(k)).wait_send()
        dz(k, z).wait_send()
    for m in range(1, nx):
        rx(m, x, xpeer(m)).wait_send()
        for zi in range(nz):
            for p in range(PIECES):
                wx(m, p, zi, x).wait_send()
            dx(m, zi, x).wait_send()
    for k in range(1, nt):
        tp(k, t).wait_send()


def per_device(nz, nx, nt, xin, gcot, fcot, scot, lam, proj, gw, gm, gs, vw, vm, vs):
    nfs = nz * nx
    rows, cg = gw.shape
    cv = vw.shape[1]
    cols = cg + cv
    depth, rank = proj.shape
    share = rank // nfs
    part = rows // PIECES
    column_lambda = jnp.repeat(lam, VDIM)[None, :]
    anywhere = pl.BlockSpec(memory_space=pl.ANY)
    dma = pltpu.SemaphoreType.DMA
    shape = jax.ShapeDtypeStruct
    like = lambda a: shape(a.shape, a.dtype)
    results = pl.pallas_call(
        functools.partial(kernel, nz, nx, nt),
        out_shape=[
            like(gw),
            like(gw),
            shape((nfs, PIECES, part, cg), bf16),
            like(gm),
            like(gs),
            like(vw),
            like(vw),
            shape((nfs, PIECES, part, cv), bf16),
            like(vm),
            like(vs),
        ],
        in_specs=[anywhere] * 4 + [pl.BlockSpec(memory_space=pltpu.VMEM)] + [anywhere] * 7,
        out_specs=[anywhere] * 10,
        scratch_shapes=[
            pltpu.VMEM(xin.shape, bf16),
            pltpu.VMEM(gcot.shape, bf16),
            pltpu.VMEM(fcot.shape, bf16),
            pltpu.VMEM(scot.shape, bf16),
            pltpu.VMEM(proj.shape, bf16),
            pltpu.VMEM(gw.shape, f32),
            pltpu.VMEM(vw.shape, f32),
            pltpu.VMEM(gm.shape, f32),
            pltpu.VMEM(gs.shape, f32),
            pltpu.VMEM(vm.shape, f32),
            pltpu.VMEM(vs.shape, f32),
            pltpu.VMEM((nfs, PIECES, part, cols), bf16),
            pltpu.VMEM((rank, cols), f32),
            pltpu.VMEM((nx, nz, share, cols), bf16),
            pltpu.VMEM((nx, nz, share, cols), bf16),
            pltpu.VMEM((nz, share, cols), bf16),
            pltpu.VMEM((nz, share, cols), bf16),
            pltpu.VMEM((nfs, share, cols), bf16),
            pltpu.VMEM((rank, cols), f32),
            pltpu.VMEM((nfs, rows, cols), f32),
            pltpu.VMEM((nt, 2, 8, 128), f32),
            pltpu.VMEM((nfs, PIECES, part, cg), bf16),
            pltpu.VMEM((nfs, PIECES, part, cv), bf16),
            pltpu.VMEM(gw.shape, f32),
            pltpu.VMEM(vw.shape, f32),
            dma((7,)),
            dma((4, CHUNKS)),
            dma((8,)),
            dma((2, PIECES)),
            dma((nz, PIECES)),
            dma((nz, PIECES)),
            dma((nx, nz, PIECES)),
            dma((nx, nz, PIECES)),
            dma((nx,)),
            dma((nx,)),
            dma((nz,)),
            dma((nz,)),
            dma((nz,)),
            dma((nz,)),
            dma((nx, nz)),
            dma((nx, nz)),
            dma((nt,)),
            dma((nt,)),
        ],
        compiler_params=pltpu.CompilerParams(
            collective_id=0, has_side_effects=True, vmem_limit_bytes=60 * 1024 * 1024
        ),
    )(xin, gcot, fcot, scot, column_lambda, proj, gw, gm, gs, vw, vm, vs)
    results = list(results)
    results[2] = results[2].reshape(depth, cg)
    results[7] = results[7].reshape(depth, cv)
    return tuple(results)


def solution(mesh):
    nz, nx = factor_fs(mesh.shape["fs"])
    split, whole = P("fs", "tp"), P(None, "tp")
    placed = (P("fs", None), split, split, split, P("tp"), P()) + (split,) * 6
    return jax.shard_map(
        functools.partial(per_device, nz, nx, mesh.shape["tp"]),
        mesh=mesh,
        in_specs=placed,
        out_specs=(split, split, whole, split, split, split, split, whole, split, split),
        check_vma=False,
    )
```

```python
import functools

import jax
import jax.numpy as jnp
from jax import lax
from jax.experimental import pallas as pl
from jax.experimental.pallas import tpu as pltpu
from jax.sharding import PartitionSpec as P

VDIM = 128
PIECES = 4
CHUNKS = 4
STEP_TOKENS = 256

moment_decay = 0.9
square_decay = 0.95
adam_floor = 1e-08
learn_rate = 0.02
rms_floor = 0.1

MESH = pl.DeviceIdType.MESH
f32, bf16 = jnp.float32, jnp.bfloat16


def factor_fs(count):
    inner = 1
    while (2 * inner) ** 2 <= count and count % (2 * inner) == 0:
        inner *= 2
    return count // inner, inner


def kernel(
    nz,
    nx,
    nt,
    x_hbm,
    gcot_hbm,
    fcot_hbm,
    scot_hbm,
    lam_ref,
    proj_hbm,
    gw_hbm,
    gm_hbm,
    gs_hbm,
    vw_hbm,
    vm_hbm,
    vs_hbm,
    wall_hbm,
    dir_hbm,
    scale_hbm,
    ngm_hbm,
    ngs_hbm,
    nvm_hbm,
    nvs_hbm,
    xv,
    gcv,
    fcv,
    scv,
    pv,
    gw,
    vw,
    gm,
    gs,
    vm,
    vs,
    wall,
    acc,
    rsrc,
    rsx,
    zsrc,
    rsz,
    dall,
    dcat,
    direct,
    sums,
    scales,
    in_sem,
    x_sem,
    out_sem,
    copy_sem,
    wz_send,
    wz_recv,
    wx_send,
    wx_recv,
    rx_send,
    rx_recv,
    rz_send,
    rz_recv,
    dz_send,
    dz_recv,
    dx_send,
    dx_recv,
    t_send,
    t_recv,
):
    nfs = nz * nx
    f = lax.axis_index("fs")
    t = lax.axis_index("tp")
    z = lax.div(f, nx)
    x = lax.rem(f, nx)
    rows, cg = gw.shape
    cv = vw.shape[1]
    cols = cg + cv
    rank = acc.shape[0]
    share = rank // nfs
    part = rows // PIECES
    tokens = x_hbm.shape[0] // CHUNKS

    def zpeer(k):
        return lax.rem(z + k, nz)

    def xpeer(k):
        return lax.rem(x + k, nx)

    barrier = pltpu.get_barrier_semaphore()
    for k in range(1, nz):
        pl.semaphore_signal(barrier, inc=1, device_id=(zpeer(k) * nx + x, t), device_id_type=MESH)
    for k in range(1, nx):
        pl.semaphore_signal(barrier, inc=1, device_id=(z * nx + xpeer(k), t), device_id_type=MESH)
    for k in range(1, nt):
        pl.semaphore_signal(barrier, inc=1, device_id=(f, lax.rem(t + k, nt)), device_id_type=MESH)

    small = [
        pltpu.make_async_copy(src, dst, in_sem.at[i])
        for i, (src, dst) in enumerate(
            [
                (gw_hbm, gw),
                (vw_hbm, vw),
                (proj_hbm, pv),
                (gm_hbm, gm),
                (gs_hbm, gs),
                (vm_hbm, vm),
                (vs_hbm, vs),
            ]
        )
    ]

    def chunk_copies(c):
        at = pl.ds(c * tokens, tokens)
        return [
            pltpu.make_async_copy(src.at[at], dst.at[at], x_sem.at[i, c])
            for i, (src, dst) in enumerate(
                [(x_hbm, xv), (gcot_hbm, gcv), (fcot_hbm, fcv), (scot_hbm, scv)]
            )
        ]

    for i in range(3):
        small[i].start()
    for c in range(CHUNKS):
        for copy in chunk_copies(c):
            copy.start()
    for i in range(3, 7):
        small[i].start()

    small[0].wait()
    small[1].wait()
    for p in range(PIECES):
        at = pl.ds(p * part, part)
        wall[f, p, :, :cg] = gw[at, :].astype(bf16)
        wall[f, p, :, cg:] = vw[at, :].astype(bf16)

    def wz(k, p, src_z):
        owner = src_z * nx + x
        return pltpu.make_async_remote_copy(
            src_ref=wall.at[owner, p],
            dst_ref=wall.at[owner, p],
            send_sem=wz_send.at[k, p],
            recv_sem=wz_recv.at[src_z, p],
            device_id=(zpeer(k) * nx + x, t),
            device_id_type=MESH,
        )

    def wx(k, p, src_z, src_x):
        owner = src_z * nx + src_x
        return pltpu.make_async_remote_copy(
            src_ref=wall.at[owner, p],
            dst_ref=wall.at[owner, p],
            send_sem=wx_send.at[k, src_z, p],
            recv_sem=wx_recv.at[src_x, src_z, p],
            device_id=(z * nx + xpeer(k), t),
            device_id_type=MESH,
        )

    def send_z(p):
        for k in range(1, nz):
            wz(k, p, z).start()

    def relay(p):
        for k in range(1, nz):
            wz(k, p, zpeer(k)).wait_recv()
            for m in range(1, nx):
                wx(m, p, zpeer(k), x).start()

    pl.semaphore_wait(barrier, (nz - 1) + (nx - 1) + (nt - 1))
    send_z(0)
    for p in range(PIECES):
        for k in range(1, nx):
            wx(k, p, z, x).start()

    small[2].wait()
    acc[...] = jnp.zeros_like(acc)
    head = lax.broadcasted_iota(jnp.int32, (1, cv), 1) // VDIM
    lam = jnp.zeros((1, cv), f32)
    for h in range(cv // VDIM):
        lam = jnp.where(head == h, lam_ref[h], lam)
    for c in range(CHUNKS):
        for copy in chunk_copies(c):
            copy.wait()

        def multiply(i, carry):
            at = pl.ds(pl.multiple_of(c * tokens + i * STEP_TOKENS, STEP_TOKENS), STEP_TOKENS)
            upper = jnp.dot(xv[at, :], pv[...], preferred_element_type=f32).astype(bf16)
            value = (fcv[at, :].astype(f32) - lam * scv[at, :].astype(f32)).astype(bf16)
            over = (((0,), (0,)), ((), ()))
            acc[:, :cg] += lax.dot_general(upper, gcv[at, :], over, preferred_element_type=f32)
            acc[:, cg:] += lax.dot_general(upper, value, over, preferred_element_type=f32)
            return carry

        lax.fori_loop(0, tokens // STEP_TOKENS, multiply, 0)

    for zi in range(nz):
        for xi in range(nx):
            at = pl.ds((zi * nx + xi) * share, share)
            rsrc[xi, zi] = acc[at, :].astype(bf16)

    def rx(k, src_x, dst_x):
        return pltpu.make_async_remote_copy(
            src_ref=rsrc.at[dst_x],
            dst_ref=rsx.at[src_x],
            send_sem=rx_send.at[k],
            recv_sem=rx_recv.at[src_x],
            device_id=(z * nx + xpeer(k), t),
            device_id_type=MESH,
        )

    for k in range(1, nx):
        rx(k, x, xpeer(k)).start()
    send_z(1)
    relay(0)
    for k in range(1, nx):
        rx(k, xpeer(k), x).wait_recv()
    for zi in range(nz):
        at = pl.ds(pl.multiple_of((zi * nx + x) * share, share), share)
        total = acc[at, :]
        for k in range(1, nx):
            total = total + rsx[xpeer(k), zi].astype(f32)
        zsrc[zi] = total.astype(bf16)

    def rz(k, src_z, dst_z):
        return pltpu.make_async_remote_copy(
            src_ref=zsrc.at[dst_z],
            dst_ref=rsz.at[src_z],
            send_sem=rz_send.at[k],
            recv_sem=rz_recv.at[src_z],
            device_id=(zpeer(k) * nx + x, t),
            device_id_type=MESH,
        )

    for k in range(1, nz):
        rz(k, z, zpeer(k)).start()
    relay(1)
    for i in range(3, 7):
        small[i].wait()
    low = zsrc[z].astype(f32)
    for k in range(1, nz):
        rz(k, zpeer(k), z).wait_recv()
        low = low + rsz[zpeer(k)].astype(f32)

    for first, second, at in ((gm, gs, slice(0, cg)), (vm, vs, slice(cg, cols))):
        mine = low[:, at]
        new_first = moment_decay * first[...] + (1.0 - moment_decay) * mine
        new_second = square_decay * second[...] + (1.0 - square_decay) * mine * mine
        first[...] = new_first
        second[...] = new_second
        dall[f, :, at] = (new_first / (jnp.sqrt(new_second) + adam_floor)).astype(bf16)

    outs = [
        pltpu.make_async_copy(src, dst, out_sem.at[i])
        for i, (src, dst) in enumerate(
            [
                (gm, ngm_hbm),
                (gs, ngs_hbm),
                (vm, nvm_hbm),
                (vs, nvs_hbm),
                (direct, dir_hbm),
                (scales, scale_hbm),
            ]
        )
    ]
    for i in range(4):
        outs[i].start()

    def dz(k, src_z):
        owner = src_z * nx + x
        return pltpu.make_async_remote_copy(
            src_ref=dall.at[owner],
            dst_ref=dall.at[owner],
            send_sem=dz_send.at[k],
            recv_sem=dz_recv.at[src_z],
            device_id=(zpeer(k) * nx + x, t),
            device_id_type=MESH,
        )

    def dx(k, src_z, src_x):
        owner = src_z * nx + src_x
        return pltpu.make_async_remote_copy(
            src_ref=dall.at[owner],
            dst_ref=dall.at[owner],
            send_sem=dx_send.at[k, src_z],
            recv_sem=dx_recv.at[src_x, src_z],
            device_id=(z * nx + xpeer(k), t),
            device_id_type=MESH,
        )

    for k in range(1, nz):
        dz(k, z).start()
    for m in range(1, nx):
        dx(m, z, x).start()
    send_z(2)
    send_z(3)
    for k in range(1, nz):
        dz(k, zpeer(k)).wait_recv()
        for m in range(1, nx):
            dx(m, zpeer(k), x).start()
    for m in range(1, nx):
        for zi in range(nz):
            dx(m, zi, xpeer(m)).wait_recv()

    relay(2)
    relay(3)
    for j in range(nfs):
        dcat[pl.ds(j * share, share), :] = dall[j].astype(f32)
    direction = dcat[...].astype(bf16)
    direct[...] = direction
    outs[4].start()

    def expand(j, squares):
        left = pv[pl.ds(pl.multiple_of(j * rows, rows), rows), :]
        block = jnp.dot(left, direction, preferred_element_type=f32)
        return squares + jnp.sum(block * block, axis=0, keepdims=True)

    squares = lax.fori_loop(0, nfs, expand, jnp.zeros((1, cols), f32))
    gate_sum = jnp.sum(squares[:, :cg], axis=1, keepdims=True)
    value_sum = jnp.sum(squares[:, cg:], axis=1, keepdims=True)
    sums[t, 0] = jnp.broadcast_to(gate_sum, (8, 128))
    sums[t, 1] = jnp.broadcast_to(value_sum, (8, 128))

    def tp(k, src_t):
        return pltpu.make_async_remote_copy(
            src_ref=sums.at[src_t],
            dst_ref=sums.at[src_t],
            send_sem=t_send.at[k],
            recv_sem=t_recv.at[src_t],
            device_id=(f, lax.rem(t + k, nt)),
            device_id_type=MESH,
        )

    for k in range(1, nt):
        tp(k, t).start()
    for k in range(1, nt):
        tp(k, lax.rem(t + k, nt)).wait_recv()
    whole = sums[0]
    for k in range(1, nt):
        whole = whole + sums[k]
    entries = nfs * rows * nt
    scales[0] = 1.0 / (jnp.sqrt(whole[0] / (entries * cg)) + rms_floor)
    scales[1] = 1.0 / (jnp.sqrt(whole[1] / (entries * cv)) + rms_floor)
    outs[5].start()

    copies = []
    for p in range(PIECES):
        for m in range(1, nx):
            for zi in range(nz):
                wx(m, p, zi, xpeer(m)).wait_recv()
        copies.append(pltpu.make_async_copy(wall.at[:, p], wall_hbm.at[:, p], copy_sem.at[p]))
        copies[-1].start()

    for copy in copies + outs:
        copy.wait()
    for k in range(1, nz):
        for p in range(PIECES):
            wz(k, p, z).wait_send()
        rz(k, z, zpeer(k)).wait_send()
        dz(k, z).wait_send()
    for m in range(1, nx):
        rx(m, x, xpeer(m)).wait_send()
        for zi in range(nz):
            for p in range(PIECES):
                wx(m, p, zi, x).wait_send()
            dx(m, zi, x).wait_send()
    for k in range(1, nt):
        tp(k, t).wait_send()


def finish_kernel(
    nz,
    nx,
    proj_hbm,
    gw_hbm,
    vw_hbm,
    wall,
    dir_hbm,
    scale_ref,
    ngm_hbm,
    ngs_hbm,
    nvm_hbm,
    nvs_hbm,
    ngw_out,
    gstep_out,
    gcopy_out,
    ngm_out,
    ngs_out,
    nvw_out,
    vstep_out,
    vcopy_out,
    nvm_out,
    nvs_out,
    pv,
    gw,
    vw,
    direct,
    gm,
    gs,
    vm,
    vs,
    gcs,
    vcs,
    gsteps,
    vsteps,
    in_sem,
    out_sem,
    copy_sem,
):
    nfs = nz * nx
    f = lax.axis_index("fs")
    rows, cg = gw.shape
    moments = [(ngm_hbm, gm, ngm_out), (ngs_hbm, gs, ngs_out), (nvm_hbm, vm, nvm_out), (nvs_hbm, vs, nvs_out)]
    loads = [(dir_hbm, direct), (proj_hbm, pv), (gw_hbm, gw), (vw_hbm, vw)]
    loads += [(src, held) for src, held, _ in moments]
    loads = [pltpu.make_async_copy(src, dst, in_sem.at[i]) for i, (src, dst) in enumerate(loads)]
    stores = [(held, dst) for _, held, dst in moments]
    stores += [(gw, ngw_out), (vw, nvw_out), (gsteps, gstep_out), (vsteps, vstep_out)]
    stores = [pltpu.make_async_copy(src, dst, out_sem.at[i]) for i, (src, dst) in enumerate(stores)]

    def put(j):
        return [
            pltpu.make_async_copy(gcs.at[j], gcopy_out.at[j], copy_sem.at[0, j]),
            pltpu.make_async_copy(vcs.at[j], vcopy_out.at[j], copy_sem.at[1, j]),
        ]

    for i in range(2):
        loads[i].start()
    for i in range(2, 8):
        loads[i].start()
    gscale = scale_ref[0, 0:1, 0:1]
    vscale = scale_ref[1, 0:1, 0:1]
    for i in range(2):
        loads[i].wait()
    direction = direct[...]

    def block(j):
        left = pv[pl.ds(pl.multiple_of(j * rows, rows), rows), :]
        return jnp.dot(left, direction, preferred_element_type=f32)

    def finish(j, carry):
        update = block(j)
        held = wall[j].astype(f32).reshape(update.shape)
        gcs[j] = (held[:, :cg] - learn_rate * (update[:, :cg] * gscale)).astype(bf16)
        vcs[j] = (held[:, cg:] - learn_rate * (update[:, cg:] * vscale)).astype(bf16)
        for copy in put(j):
            copy.start()
        return carry

    lax.fori_loop(0, nfs, finish, 0)
    for i in range(2, 8):
        loads[i].wait()
    for i in range(4):
        stores[i].start()
    mine = block(f)
    gstep = mine[:, :cg] * gscale
    vstep = mine[:, cg:] * vscale
    gsteps[...] = gstep
    vsteps[...] = vstep
    gw[...] = gw[...] - learn_rate * gstep
    vw[...] = vw[...] - learn_rate * vstep
    for i in range(4, 8):
        stores[i].start()
    for j in range(nfs):
        for copy in put(j):
            copy.wait()
    for copy in stores:
        copy.wait()


def per_device(nz, nx, nt, xin, gcot, fcot, scot, lam, proj, gw, gm, gs, vw, vm, vs):
    nfs = nz * nx
    rows, cg = gw.shape
    cv = vw.shape[1]
    cols = cg + cv
    depth, rank = proj.shape
    share = rank // nfs
    part = rows // PIECES
    anywhere = pl.BlockSpec(memory_space=pl.ANY)
    pinned = pl.BlockSpec(memory_space=pl.ANY)
    dma = pltpu.SemaphoreType.DMA
    shape = jax.ShapeDtypeStruct
    like = lambda a: shape(a.shape, a.dtype)
    vmem = lambda a: pltpu.VMEM(a.shape, a.dtype)
    wall, direction, scale, *moments = pl.pallas_call(
        functools.partial(kernel, nz, nx, nt),
        out_shape=[
            shape((nfs, PIECES, part, cols), bf16),
            shape((rank, cols), bf16),
            shape((2, 8, 128), f32),
            like(gm),
            like(gs),
            like(vm),
            like(vs),
        ],
        in_specs=[pinned] * 4 + [pl.BlockSpec(memory_space=pltpu.SMEM)] + [pinned] * 7,
        out_specs=[anywhere] * 7,
        scratch_shapes=[
            vmem(xin),
            vmem(gcot),
            vmem(fcot),
            vmem(scot),
            vmem(proj),
            vmem(gw),
            vmem(vw),
            vmem(gm),
            vmem(gs),
            vmem(vm),
            vmem(vs),
            pltpu.VMEM((nfs, PIECES, part, cols), bf16),
            pltpu.VMEM((rank, cols), f32),
            pltpu.VMEM((nx, nz, share, cols), bf16),
            pltpu.VMEM((nx, nz, share, cols), bf16),
            pltpu.VMEM((nz, share, cols), bf16),
            pltpu.VMEM((nz, share, cols), bf16),
            pltpu.VMEM((nfs, share, cols), bf16),
            pltpu.VMEM((rank, cols), f32),
            pltpu.VMEM((rank, cols), bf16),
            pltpu.VMEM((nt, 2, 8, 128), f32),
            pltpu.VMEM((2, 8, 128), f32),
            dma((7,)),
            dma((4, CHUNKS)),
            dma((6,)),
            dma((PIECES,)),
            dma((nz, PIECES)),
            dma((nz, PIECES)),
            dma((nx, nz, PIECES)),
            dma((nx, nz, PIECES)),
            dma((nx,)),
            dma((nx,)),
            dma((nz,)),
            dma((nz,)),
            dma((nz,)),
            dma((nz,)),
            dma((nx, nz)),
            dma((nx, nz)),
            dma((nt,)),
            dma((nt,)),
        ],
        compiler_params=pltpu.CompilerParams(
            collective_id=0, has_side_effects=True, vmem_limit_bytes=60 * 1024 * 1024
        ),
    )(xin, gcot, fcot, scot, lam, proj, gw, gm, gs, vw, vm, vs)
    results = pl.pallas_call(
        functools.partial(finish_kernel, nz, nx),
        out_shape=[
            like(gw),
            like(gw),
            shape((nfs, rows, cg), bf16),
            like(gm),
            like(gs),
            like(vw),
            like(vw),
            shape((nfs, rows, cv), bf16),
            like(vm),
            like(vs),
        ],
        in_specs=[pinned] * 3 + [pl.BlockSpec(memory_space=pltpu.VMEM), anywhere] + [pl.BlockSpec(memory_space=pltpu.VMEM)] + [anywhere] * 4,
        out_specs=[anywhere] * 10,
        scratch_shapes=[
            vmem(proj),
            vmem(gw),
            vmem(vw),
            vmem(direction),
            vmem(gm),
            vmem(gs),
            vmem(vm),
            vmem(vs),
            pltpu.VMEM((nfs, rows, cg), bf16),
            pltpu.VMEM((nfs, rows, cv), bf16),
            vmem(gw),
            vmem(vw),
            dma((8,)),
            dma((8,)),
            dma((2, nfs)),
        ],
        compiler_params=pltpu.CompilerParams(vmem_limit_bytes=60 * 1024 * 1024),
    )(proj, gw, vw, wall, direction, scale, *moments)
    results = list(results)
    results[2] = results[2].reshape(depth, cg)
    results[7] = results[7].reshape(depth, cv)
    return tuple(results)


def solution(mesh):
    nz, nx = factor_fs(mesh.shape["fs"])
    split, whole = P("fs", "tp"), P(None, "tp")
    placed = (P("fs", None), split, split, split, P("tp"), P()) + (split,) * 6
    return jax.shard_map(
        functools.partial(per_device, nz, nx, mesh.shape["tp"]),
        mesh=mesh,
        in_specs=placed,
        out_specs=(split, split, whole, split, split, split, split, whole, split, split),
        check_vma=False,
    )
```
